128 devices in a mesh: fs: 16 (over z, y), tp: 8 (over x, core).
Axes of the slice: x: 4, y: 4, z: 4, core: 2. Of those that a mesh axis runs over, the one named last changes fastest.
Arguments:
- tokens: bfloat16 [32768, 2048], P('fs'), may hold values from -6 to 6
- norm_gain: float32 [2048], replicated, may hold values from 0.1 to 1.9
- gate_weight: bfloat16 [2048, 5632], P('fs', 'tp'), may hold values from -0.125 to 0.125
- up_weight: bfloat16 [2048, 5632], P('fs', 'tp'), may hold values from -0.125 to 0.125
- down_weight: bfloat16 [5632, 2048], P('tp', 'fs'), may hold values from -0.078125 to 0.078125
Outputs:
- mixed: bfloat16 [32768, 2048], P(('fs', 'tp'))
The draws below stay inside these ranges and needn't reach their ends.
All inputs are finite; a program needn't handle non-finite values.
Results may differ from the reference program's by a relative error of at most 0.014.
Values may be sent and summed in bfloat16 or wider, within the bound.
A program may use at most 128 MiB of HBM per device.

```python
import jax
import jax.numpy as jnp
from jax import lax

D = 2048
FF = 5632
TOKENS = 32768
N_FS = 16
N_TP = 8


def block_scale(own_key, extent, cuts, low, high):
    loudness = 1.0
    for axis_at, blocks in cuts:
        heights = jax.random.uniform(jax.random.fold_in(jax.random.fold_in(own_key, 6), axis_at), (blocks,), jnp.float32, low / len(cuts), high / len(cuts))
        loudness = loudness * jnp.repeat(jnp.exp(heights), extent[axis_at] // blocks).reshape((-1,) + (1,) * (len(extent) - 1 - axis_at))
    return loudness


def gaussian(key, dims, spread, limit, shards=(), kind=jnp.bfloat16):
    values = jax.random.normal(key, dims, jnp.float32) * spread
    if len(shards) > 0:
        values = block_scale(key, dims, shards, -0.22, 0.18) * values
    return jnp.clip(values, min=-limit, max=limit).astype(kind)


def setup_inputs(seed: int = 0) -> dict:
    splits = jax.random.split(jax.random.key(seed), 6)
    tokens = gaussian(splits[0], (TOKENS, D), 1.0, 6.0, ((0, 16),))
    norm_gain = jnp.clip(1.0 + 0.18 * jax.random.normal(splits[1], (D,), jnp.float32), 0.1, 1.9)
    gate_weight = gaussian(splits[2], (D, FF), D ** -0.5, 0.125, ((0, 16), (1, 8)))
    up_weight = gaussian(splits[3], (D, FF), D ** -0.5, 0.125, ((0, 16), (1, 8)))
    down_weight = gaussian(splits[4], (FF, D), FF ** -0.5, 0.078125, ((0, 8), (1, 16)))
    return {"tokens": tokens, "norm_gain": norm_gain, "gate_weight": gate_weight, "up_weight": up_weight, "down_weight": down_weight}


def block_rows(xrows, norm_gain, gate_weight, up_weight, down_weight):
    xf = xrows.astype(jnp.float32)
    scale = lax.rsqrt(lax.optimization_barrier(jnp.mean(xf * xf, axis=-1, keepdims=True)) + 1e-06)
    normed = (xf * scale * norm_gain).astype(jnp.bfloat16)
    gate = jnp.dot(normed, gate_weight, preferred_element_type=jnp.float32)
    up = jnp.dot(normed, up_weight, preferred_element_type=jnp.float32)
    hidden = (jax.nn.silu(gate) * up).astype(jnp.bfloat16)
    width = FF // N_TP

    def add_block(total, index):
        start = (index * width).astype(jnp.int32)
        left = lax.dynamic_slice_in_dim(hidden, start, width, 1)
        right = lax.dynamic_slice_in_dim(down_weight, start, width, 0)
        part = jnp.dot(left, right, preferred_element_type=jnp.float32).astype(jnp.bfloat16)
        return (total + part.astype(jnp.float32), None)
    total, unused = lax.scan(add_block, jnp.zeros((xrows.shape[0], D), jnp.float32), jnp.arange(N_TP, dtype=jnp.int32))
    return total.astype(jnp.bfloat16)

def reference(tokens, norm_gain, gate_weight, up_weight, down_weight):
    blocks = tokens.reshape(N_FS, TOKENS // N_FS, D)
    result = lax.map(lambda rows: block_rows(rows, norm_gain, gate_weight, up_weight, down_weight), blocks)
    return result.reshape(TOKENS, D)
```

```python
import heapq

import jax
import jax.numpy as jnp
from jax import lax
from jax.experimental import pallas as pl
from jax.experimental.pallas import tpu as pltpu
from jax.sharding import PartitionSpec as P

D = 2048
N_FS = 16
F = 704
FM = 640
TT = 256
GQ = 32
DQ = 176
LINKS = ("y+", "y-", "z+", "z-")
FIRST = {"y+": (0, 1, 2, 3), "y-": (1, 0, 3, 2), "z+": (2, 3, 0, 1), "z-": (3, 2, 1, 0)}


def near(d):
    return (d + 1) % 4 - 1


def onward(q, dz, dy):
    first, second = ("y", "z") if q < 2 else ("z", "y")
    sign = "+" if q % 2 == 0 else "-"
    a, b = (dy, dz) if q < 2 else (dz, dy)
    came = {-1: "+", 1: "-"}
    if b == 0:
        out = [first + sign] if came.get(a) == sign else []
        return out + [second + sign, second + ("-" if sign == "+" else "+")]
    return [second + sign] if came.get(b) == sign else []


def seen_from(link, dz, dy):
    step = 1 if link[1] == "+" else -1
    return (near(dz - step), dy) if link[0] == "z" else (dz, near(dy - step))


def gather_events(unit, lat, backlog):
    free = {l: 0.0 for l in LINKS}
    count = {l: 0 for l in LINKS}
    heap = {l: [] for l in LINKS}
    flying, n = [], 0

    def offer(l, k, q, dz, dy):
        nonlocal n
        n += 1
        heapq.heappush(heap[l], (k == "d", n, k, q, dz, dy))

    def top_up(t):
        nonlocal n
        sends = []
        for l in LINKS:
            while heap[l] and free[l] - t < backlog and (heap[l][0][2] == "g" or count[l] >= 15):
                _, _, k, q, dz, dy = heapq.heappop(heap[l])
                count[l] += 1
                n += 1
                free[l] = max(t, free[l]) + unit[k]
                sends.append((l, k, q, dz, dy))
                heapq.heappush(flying, (free[l] + lat, n, k, q, *seen_from(l, dz, dy)))
        return sends

    for l in LINKS:
        for k in "gd":
            for q in FIRST[l]:
                offer(l, k, q, 0, 0)
    events = [(0.0, None, top_up(0.0))]
    while flying:
        t, _, k, q, dz, dy = heapq.heappop(flying)
        for l in onward(q, dz, dy):
            offer(l, k, q, dz, dy)
        events.append((t, (k, q, dz, dy), top_up(t)))
    return events


def make_plan(unit={"g": 1.93, "d": 0.97}, lat=2.0, backlog=6.0, sib=1.8):
    events = gather_events(unit, lat, backlog)
    done, left = {("g", 0, 0): 0.0, ("d", 0, 0): 0.0}, {}
    for t, what, _ in events[1:]:
        k, q, dz, dy = what
        left[(k, dz, dy)] = left.get((k, dz, dy), 0) + 1
        if left[(k, dz, dy)] == 4:
            done[(k, dz, dy)] = t
    order = {k: [key[1:] for key in sorted((key for key in done if key[0] == k), key=lambda key: done[key])] for k in "gd"}
    assert len(order["g"]) == 16 and len(order["d"]) == 16
    steps = [order["g"][4 * i : 4 * i + 4] for i in range(4)]
    groups = [order["d"][:1]] + [order["d"][1 + 2 * i : 3 + 2 * i] for i in range(7)] + [order["d"][15:]]
    work = [(1.5, 1.2, ("norm", b)) for b in range(4)]
    for i in range(3):
        ready = max(done[("g", *s)] for s in steps[i])
        work.append((ready, 2.2, ("acc", i, 0)))
        work.append((ready + sib, 2.2, ("acc", i, 1)))
        work.append((ready + sib, 0.5, ("acc", i, 2)))
    ready = max(done[("g", *s)] for s in steps[3]) + sib
    for b in range(4):
        work += [(ready, 1.2, ("fin", b)), (ready, 0.3, ("down", 0, b))]
    for i in range(1, len(groups)):
        ready = max(done[("d", *s)] for s in groups[i]) + sib
        work += [(ready, 0.4, ("down", i, b)) for b in range(4)]
    plan, now, w, got = [], 0.0, 0, {}
    plan += [("send", *s) for s in events[0][2]] + [("pass", "g", 0, 0), ("pass", "d", 0, 0)]
    for t, what, sends in events[1:]:
        while w < len(work) and max(now, work[w][0]) + work[w][1] <= t + 0.6:
            plan.append(work[w][2])
            now = max(now, work[w][0]) + work[w][1]
            w += 1
        k, q, dz, dy = what
        plan.append(("recv", *what))
        now = max(now, t)
        plan += [("send", *s) for s in sends]
        got[(k, dz, dy)] = got.get((k, dz, dy), 0) + 1
        if got[(k, dz, dy)] == 4:
            plan.append(("pass", k, dz, dy))
    plan += [item[2] for item in work[w:]]
    return plan, steps, groups


def kernel(tok_hbm, gain_ref, gu_hbm, dn_hbm, out_ref, tok, normed, wgu, wdn, acc, hid, far_s, far_r, near_p, near_m,
           in_m, in_n, own, loc_sem, tok_sem, g_recv, d_recv, gs_recv, ds_recv, x_recv, send_sem):
    plan, steps, groups = make_plan()
    fs, tp = lax.axis_index("fs"), lax.axis_index("tp")
    z, y = fs // 4, fs % 4
    x, core = tp // 2, tp % 2

    def dev(link):
        step = 1 if link[1] == "+" else 3
        if link[0] == "z":
            return {"fs": ((z + step) % 4) * 4 + y, "tp": tp}
        if link[0] == "y":
            return {"fs": z * 4 + (y + step) % 4, "tp": tp}
        if link[0] == "x":
            return {"fs": fs, "tp": ((x + step) % 4) * 2 + core}
        return {"fs": fs, "tp": x * 2 + 1 - core}

    peers = {l: dev(l) for l in LINKS + ("x+", "x-", "c+")}
    shard = {(dz, dy): ((z + dz + 4) % 4) * 4 + (y + dy + 4) % 4 for dz in range(-1, 3) for dy in range(-1, 3)}

    def label(dz, dy):
        return (dz + 1) * 4 + dy + 1

    def rows(dz, dy, at, size):
        return pl.ds(pl.multiple_of(shard[(dz, dy)] * 128 + at, size), size)

    def piece(k, q, dz, dy):
        if k == "g":
            return wgu.at[0, rows(dz, dy, q * GQ, GQ), :]
        return wdn.at[shard[(dz, dy)], 0, pl.ds(q * DQ, DQ), :]

    def copy_piece(link, k, q, dz, dy):
        there = seen_from(link, dz, dy)
        ref = piece(k, q, dz, dy)
        sems, s = (g_recv, 0) if k == "g" else (d_recv, 1)
        return pltpu.make_async_remote_copy(
            src_ref=ref, dst_ref=ref, send_sem=send_sem.at[s], recv_sem=sems.at[q * 16 + label(*there)],
            device_id=peers[link], device_id_type=pl.DeviceIdType.MESH)

    def recv_piece(k, q, dz, dy):
        ref = piece(k, q, dz, dy)
        sem = (g_recv if k == "g" else d_recv).at[q * 16 + label(dz, dy)]
        pltpu.make_async_copy(ref, ref, sem).wait()

    def whole(k, slot, dz, dy):
        if k == "g":
            return wgu.at[slot, rows(dz, dy, 0, 128), :]
        return wdn.at[shard[(dz, dy)], slot]

    def pass_shard(k, dz, dy):
        sems, s = (gs_recv, 2) if k == "g" else (ds_recv, 3)
        pltpu.make_async_remote_copy(
            src_ref=whole(k, 0, dz, dy), dst_ref=whole(k, 1, dz, dy), send_sem=send_sem.at[s],
            recv_sem=sems.at[label(dz, dy)], device_id=peers["c+"], device_id_type=pl.DeviceIdType.MESH).start()

    passed = set()

    def need_passed(k, shards):
        for s in shards:
            if (k, *s) not in passed:
                passed.add((k, *s))
                ref = whole(k, 1, *s)
                pltpu.make_async_copy(ref, ref, (gs_recv if k == "g" else ds_recv).at[label(*s)]).wait()

    own_g = pltpu.make_async_copy(gu_hbm, whole("g", 0, 0, 0), loc_sem.at[0])
    own_d = pltpu.make_async_copy(dn_hbm, whole("d", 0, 0, 0), loc_sem.at[1])
    own_g.start()
    own_d.start()

    def tok_copy(b):
        to = (x + (2, 1, 3, 0)[b]) % 4
        at = pl.multiple_of((to * 2 + core) * TT, TT)
        return pltpu.make_async_copy(tok_hbm.at[pl.ds(at, TT), :], tok.at[b], tok_sem.at[b])

    for b in range(4):
        tok_copy(b).start()

    barrier = pltpu.get_barrier_semaphore()
    for peer in peers.values():
        pl.semaphore_signal(barrier, inc=1, device_id=peer, device_id_type=pl.DeviceIdType.MESH)
    pl.semaphore_wait(barrier, len(peers))
    own_g.wait()
    own_d.wait()

    def norm(b):
        tok_copy(b).wait()

        @pl.loop(0, TT // 16)
        def _(i):
            r = pl.ds(pl.multiple_of(i * 16, 16), 16)
            v = tok[b, r, :].astype(jnp.float32)
            scale = lax.rsqrt(jnp.mean(v * v, axis=-1, keepdims=True) + 1e-06)
            n = (v * scale * gain_ref[...]).astype(jnp.bfloat16)
            to = pl.ds(pl.multiple_of(b * TT + i * 16, 16), 16)
            for s in range(N_FS):
                normed[s, to, :] = n[:, s * 128 : (s + 1) * 128]

    def lhs(step, r):
        return jnp.concatenate([normed[shard[s], r, :] for s in step], axis=1)

    def rhs(step, tile):
        def part(s):
            if tile < 10:
                return wgu[tile // 5, rows(*s, 0, 128), (tile % 5) * 256 : (tile % 5) * 256 + 256]
            return jnp.concatenate([wgu[c, rows(*s, 0, 128), 2 * FM : 2 * F] for c in range(2)], axis=1)

        return jnp.concatenate([part(s) for s in step], axis=0)

    def accumulate(i, part):
        step = steps[i]
        if part > 0:
            need_passed("g", step)
        tiles = (range(0, 5), range(5, 10), range(10, 11))[part]

        @pl.loop(0, 2)
        def _(h):
            r = pl.ds(pl.multiple_of(h * 512, 512), 512)
            left = lhs(step, r)
            for tile in tiles:
                prod = jnp.dot(left, rhs(step, tile), preferred_element_type=jnp.float32)
                if i == 0:
                    acc[tile, r, :] = prod
                else:
                    acc[tile, r, :] += prod

    def gated(g, u):
        return (g / (1.0 + jnp.exp(-g)) * u).astype(jnp.bfloat16)

    def finish(b):
        need_passed("g", steps[3])
        r = pl.ds(b * TT, TT)
        left = lhs(steps[3], r)
        for tile in range(11):
            v = acc[tile, r, :] + jnp.dot(left, rhs(steps[3], tile), preferred_element_type=jnp.float32)
            a, c = v[:, :128], v[:, 128:]
            if tile == 10:
                low = lax.broadcasted_iota(jnp.int32, a.shape, 1) < 64
                a, c = jnp.where(low, a, pltpu.roll(c, 64, 1)), jnp.where(low, pltpu.roll(a, 64, 1), c)
            hid[r, tile * 128 : tile * 128 + 128] = gated(a, c)

    starts = [sum(len(g) for g in groups[:i]) for i in range(len(groups))]

    def half(ref, i, h):
        return ref.at[pl.ds(starts[i], len(groups[i])), pl.ds(h * 128, 128), :]

    def x_copy(kind, i, h):
        src, dst, link = {
            ("far", 0): (far_s, far_r, "x+"), ("far", 1): (far_s, far_r, "x-"),
            ("m", 0): (near_m, in_m, "x-"), ("m", 1): (near_p, in_m, "x+"),
            ("n", 0): (near_p, in_n, "x+"), ("n", 1): (near_m, in_n, "x-"),
        }[(kind, h)]
        c = ("far", "m", "n").index(kind)
        return pltpu.make_async_remote_copy(
            src_ref=half(src, i, h), dst_ref=half(dst, i, h), send_sem=send_sem.at[4 + c],
            recv_sem=x_recv.at[(c * 9 + i) * 2 + h], device_id=peers[link], device_id_type=pl.DeviceIdType.MESH)

    def x_wait(kind, i, h):
        dst = {"far": far_r, "m": in_m, "n": in_n}[kind]
        c = ("far", "m", "n").index(kind)
        ref = half(dst, i, h)
        pltpu.make_async_copy(ref, ref, x_recv.at[(c * 9 + i) * 2 + h]).wait()

    def down(i, b):
        need_passed("d", groups[i])

        def part(s):
            w = [(c, lo, hi) for lo, hi in ((0, FM), (FM, F)) for c in range(2)]
            return jnp.concatenate([wdn[shard[s], c, lo:hi, :] for c, lo, hi in w], axis=0)

        right = [part(s) for s in groups[i]]
        right = right[0] if len(right) == 1 else jnp.concatenate(right, axis=1)
        prod = jnp.dot(hid[pl.ds(b * TT, TT), :], right, preferred_element_type=jnp.float32)
        to = (far_s, near_p, near_m, own)[b]
        for j in range(len(groups[i])):
            to[starts[i] + j, :, :] = prod[:, j * 128 : j * 128 + 128].astype(to.dtype)
        if b == 0:
            x_copy("far", i, 0).start()
            x_copy("far", i, 1).start()
        if b == 1:
            x_copy("m", i, 1).start()
        if b == 2:
            x_copy("m", i, 0).start()

    for op, *a in plan:
        if op == "send":
            copy_piece(*a).start()
        elif op == "recv":
            recv_piece(*a)
        elif op == "pass":
            pass_shard(*a)
        elif op == "norm":
            norm(*a)
        elif op == "acc":
            accumulate(*a)
        elif op == "fin":
            finish(*a)
        else:
            down(*a)

    f32 = jnp.float32
    for i in range(len(groups)):
        for h in range(2):
            x_wait("far", i, h)
            ref = (near_p, near_m)[h]
            at = (pl.ds(starts[i], len(groups[i])), pl.ds(h * 128, 128), slice(None))
            ref[at] = (ref[at].astype(f32) + far_r[at].astype(f32)).astype(jnp.bfloat16)
            x_copy("n", i, h).start()
    for i in range(len(groups)):
        for h in range(2):
            x_wait("m", i, h)
            x_wait("n", i, h)
        for j, s in enumerate(groups[i]):
            u = starts[i] + j
            total = own[u] + in_m[u].astype(f32) + in_n[u].astype(f32)
            out_ref[:, pl.ds(pl.multiple_of(shard[s] * 128, 128), 128)] = total.astype(jnp.bfloat16)

    sent = (wgu.at[0, pl.ds(0, 1920), :], wdn.at[pl.ds(0, 15), 0], wgu.at[0], wdn.at[:, 0], far_s, near_p, near_m)
    for i, ref in enumerate(sent):
        pltpu.make_async_copy(ref, ref, send_sem.at[i]).wait()


def per_device(tokens, norm_gain, gate_weight, up_weight, down_weight):
    cols = []
    for lo in range(0, F, 128):
        hi = min(lo + 128, F)
        cols += [gate_weight[:, lo:hi], up_weight[:, lo:hi]]
    gu = jnp.concatenate(cols, axis=1)
    vmem, dma = pltpu.VMEM, pltpu.SemaphoreType.DMA
    bf, f32 = jnp.bfloat16, jnp.float32
    unit = (N_FS, TT, 128)
    any_spec = pl.BlockSpec(memory_space=pl.ANY)
    return pl.pallas_call(
        kernel,
        out_shape=jax.ShapeDtypeStruct((TT, D), bf),
        in_specs=[any_spec, pl.BlockSpec(memory_space=pltpu.VMEM), any_spec, any_spec],
        out_specs=pl.BlockSpec(memory_space=pltpu.VMEM),
        scratch_shapes=[
            vmem((4, TT, D), bf), vmem((N_FS, 4 * TT, 128), bf), vmem((2, D, 2 * F), bf), vmem((N_FS, 2, F, 128), bf),
            vmem((11, 4 * TT, 256), f32), vmem((4 * TT, 2 * F), bf),
            vmem(unit, bf), vmem(unit, bf), vmem(unit, bf), vmem(unit, bf), vmem(unit, bf), vmem(unit, bf), vmem(unit, f32),
            dma((2,)), dma((4,)), dma((64,)), dma((64,)), dma((16,)), dma((16,)), dma((54,)), dma((7,)),
        ],
        compiler_params=pltpu.CompilerParams(collective_id=0, has_side_effects=True, vmem_limit_bytes=63 * 2**20),
        name="ffn",
    )(tokens, norm_gain.reshape(1, D), gu, down_weight)


def solution(mesh):
    placed = (P("fs", None), P(), P("fs", "tp"), P("fs", "tp"), P("tp", "fs"))
    return jax.shard_map(
        per_device, mesh=mesh, in_specs=placed, out_specs=P(("fs", "tp"), None), check_vma=False
    )
```

```python
import heapq

import jax
import jax.numpy as jnp
from jax import lax
from jax.experimental import pallas as pl
from jax.experimental.pallas import tpu as pltpu
from jax.sharding import PartitionSpec as P

D = 2048
N_FS = 16
F = 704
FM = 640
TT = 256
GQ = 352
DQ = 176
RANK = {1: 1, 2: 2, 4: 3, 5: 4, 8: 5}
LINKS = ("y+", "y-", "z+", "z-")
FIRST = {"y+": (0, 1, 2, 3), "y-": (1, 0, 3, 2), "z+": (2, 3, 0, 1), "z-": (3, 2, 1, 0)}


def near(d):
    return (d + 1) % 4 - 1


def onward(q, dz, dy):
    first, second = ("y", "z") if q < 2 else ("z", "y")
    sign = "+" if q % 2 == 0 else "-"
    a, b = (dy, dz) if q < 2 else (dz, dy)
    came = {-1: "+", 1: "-"}
    if b == 0:
        out = [first + sign] if came.get(a) == sign else []
        return out + [second + sign, second + ("-" if sign == "+" else "+")]
    return [second + sign] if came.get(b) == sign else []


def seen_from(link, dz, dy):
    step = 1 if link[1] == "+" else -1
    return (near(dz - step), dy) if link[0] == "z" else (dz, near(dy - step))


def gather_events(unit, lat, backlog):
    free = {l: 0.0 for l in LINKS}
    count = {l: 0 for l in LINKS}
    heap = {l: [] for l in LINKS}
    flying, n = [], 0

    def offer(l, k, q, dz, dy):
        nonlocal n
        n += 1
        tz, ty = seen_from(l, dz, dy)
        early = tz == 0 if q < 2 else ty == 0
        heapq.heappush(heap[l], (k == "d", 0 if early else RANK[tz * tz + ty * ty], n, k, q, dz, dy))

    def top_up(t):
        nonlocal n
        sends = []
        for l in LINKS:
            while heap[l] and free[l] - t < backlog and (heap[l][0][0] == 0 or count[l] >= 15):
                _, _, _, k, q, dz, dy = heapq.heappop(heap[l])
                count[l] += 1
                n += 1
                free[l] = max(t, free[l]) + unit[k]
                sends.append((l, k, q, dz, dy))
                heapq.heappush(flying, (free[l] + lat, n, k, q, *seen_from(l, dz, dy)))
        return sends

    for l in LINKS:
        for k in "gd":
            for q in FIRST[l]:
                offer(l, k, q, 0, 0)
    events = [(0.0, None, top_up(0.0))]
    while flying:
        t, _, k, q, dz, dy = heapq.heappop(flying)
        for l in onward(q, dz, dy):
            offer(l, k, q, dz, dy)
        events.append((t, (k, q, dz, dy), top_up(t)))
    return events


def make_plan(unit={"g": 1.93, "d": 0.97}, lat=2.2, backlog=6.0, sib=1.8, sizes=(5, 6, 2, 3), margin=0.4, log=None):
    events = gather_events(unit, lat, backlog)
    done, left = {("g", 0, 0): 0.0, ("d", 0, 0): 0.0}, {}
    for t, what, _ in events[1:]:
        k, q, dz, dy = what
        left[(k, dz, dy)] = left.get((k, dz, dy), 0) + 1
        if left[(k, dz, dy)] == 4:
            done[(k, dz, dy)] = t + margin
    order = {k: [key[1:] for key in sorted((key for key in done if key[0] == k), key=lambda key: done[key])] for k in "gd"}
    assert len(order["g"]) == 16 and len(order["d"]) == 16
    steps = [order["g"][sum(sizes[:i]) : sum(sizes[: i + 1])] for i in range(len(sizes))]
    groups = [order["d"][:1]] + [order["d"][1 + 2 * i : 3 + 2 * i] for i in range(7)] + [order["d"][15:]]
    last = len(steps) - 1
    work = [(0.0, 1.9, ("norm", b)) for b in range(4)]
    for i in range(last):
        ready = max(done[("g", *s)] for s in steps[i])
        cost = 0.43 * len(steps[i])
        work.append((ready, cost, ("acc", i, 0)))
        work.append((ready + sib, cost, ("acc", i, 1)))
        work.append((ready + sib, cost * 0.35, ("acc", i, 2)))
    cost = 0.45 + 0.15 * len(steps[last])
    ready = max(done[("g", *s)] for s in steps[last]) + sib
    for b in range(4):
        work += [(ready, cost, ("fin", b)), (ready, 0.38, ("down", 0, b))]
    for i in range(1, len(groups)):
        ready = max(done[("d", *s)] for s in groups[i]) + sib
        if i == 1:
            work += [(ready, 0.55, ("down", i, b)) for b in range(4)]
        else:
            work.append((ready, 1.8, ("down", i, None)))
        if i == 2:
            work.append((ready, 0.1, ("add", 0)))
    work += [(0.0, 0.1, ("add", i)) for i in range(1, len(groups))]
    plan, now, got, events = [], 0.0, {}, events[::-1]
    plan += [("send", *s) for s in events.pop()[2]] + [("pass", "g", 0, 0), ("pass", "d", 0, 0)]
    work = work[::-1]
    while events or work:
        if events and (not work or events[-1][0] + margin <= max(now, work[-1][0])):
            t, what, sends = events.pop()
            k, q, dz, dy = what
            plan.append(("recv", *what))
            now = max(now, t + margin)
            plan += [("send", *s) for s in sends]
            got[(k, dz, dy)] = got.get((k, dz, dy), 0) + 1
            if got[(k, dz, dy)] == 4:
                plan.append(("pass", k, dz, dy))
        else:
            ready, cost, op = work.pop()
            now = max(now, ready)
            plan.append(op)
            if log is not None:
                log.append((round(now, 1), op))
            now += cost
    return plan, steps, groups


def kernel(tok_hbm, gain_ref, gate_hbm, up_hbm, dn_hbm, out_ref, tok, normed, wgu, wdn, acc, hid, far_s, far_r, near_p, near_m,
           in_m, in_n, own, loc_sem, tok_sem, g_recv, d_recv, gs_recv, ds_recv, x_recv, send_sem):
    plan, steps, groups = make_plan()
    fs, tp = lax.axis_index("fs"), lax.axis_index("tp")
    z, y = fs // 4, fs % 4
    x, core = tp // 2, tp % 2

    def dev(link):
        step = 1 if link[1] == "+" else 3
        if link[0] == "z":
            return {"fs": ((z + step) % 4) * 4 + y, "tp": tp}
        if link[0] == "y":
            return {"fs": z * 4 + (y + step) % 4, "tp": tp}
        if link[0] == "x":
            return {"fs": fs, "tp": ((x + step) % 4) * 2 + core}
        return {"fs": fs, "tp": x * 2 + 1 - core}

    peers = {l: dev(l) for l in LINKS + ("x+", "x-", "c+")}
    shard = {(dz, dy): ((z + dz + 4) % 4) * 4 + (y + dy + 4) % 4 for dz in range(-1, 3) for dy in range(-1, 3)}

    def label(dz, dy):
        return (dz + 1) * 4 + dy + 1

    def piece(k, q, dz, dy):
        if k == "g":
            return wgu.at[shard[(dz, dy)], 0, pl.ds(q * GQ, GQ), :]
        return wdn.at[shard[(dz, dy)], 0, pl.ds(q * DQ, DQ), :]

    def copy_piece(link, k, q, dz, dy):
        there = seen_from(link, dz, dy)
        ref = piece(k, q, dz, dy)
        sems, s = (g_recv, 0) if k == "g" else (d_recv, 1)
        return pltpu.make_async_remote_copy(
            src_ref=ref, dst_ref=ref, send_sem=send_sem.at[s], recv_sem=sems.at[q * 16 + label(*there)],
            device_id=peers[link], device_id_type=pl.DeviceIdType.MESH)

    def recv_piece(k, q, dz, dy):
        ref = piece(k, q, dz, dy)
        sem = (g_recv if k == "g" else d_recv).at[q * 16 + label(dz, dy)]
        pltpu.make_async_copy(ref, ref, sem).wait()

    def whole(k, slot, dz, dy):
        return (wgu if k == "g" else wdn).at[shard[(dz, dy)], slot]

    def pass_shard(k, dz, dy):
        sems, s = (gs_recv, 2) if k == "g" else (ds_recv, 3)
        pltpu.make_async_remote_copy(
            src_ref=whole(k, 0, dz, dy), dst_ref=whole(k, 1, dz, dy), send_sem=send_sem.at[s],
            recv_sem=sems.at[label(dz, dy)], device_id=peers["c+"], device_id_type=pl.DeviceIdType.MESH).start()

    passed = set()

    def need_passed(k, shards):
        for s in shards:
            if (k, *s) not in passed:
                passed.add((k, *s))
                ref = whole(k, 1, *s)
                pltpu.make_async_copy(ref, ref, (gs_recv if k == "g" else ds_recv).at[label(*s)]).wait()

    barrier = pltpu.get_barrier_semaphore()
    for peer in peers.values():
        pl.semaphore_signal(barrier, inc=1, device_id=peer, device_id_type=pl.DeviceIdType.MESH)
    own_g = pltpu.make_async_copy(gate_hbm, whole("g", 0, 0, 0).at[pl.ds(0, F), :], loc_sem.at[0])
    own_u = pltpu.make_async_copy(up_hbm, whole("g", 0, 0, 0).at[pl.ds(F, F), :], loc_sem.at[1])
    own_d = pltpu.make_async_copy(dn_hbm, whole("d", 0, 0, 0), loc_sem.at[2])
    own_g.start()
    own_u.start()
    own_d.start()

    def tok_copy(b):
        to = (x + (2, 1, 3, 0)[b]) % 4
        at = pl.multiple_of((to * 2 + core) * TT, TT)
        return pltpu.make_async_copy(tok_hbm.at[pl.ds(at, TT), :], tok.at[b], tok_sem.at[b])

    own_g.wait()
    own_u.wait()
    own_d.wait()
    for b in range(4):
        tok_copy(b).start()
    pl.semaphore_wait(barrier, len(peers))

    def norm(b):
        tok_copy(b).wait()

        @pl.loop(0, TT // 16)
        def _(i):
            r = pl.ds(pl.multiple_of(i * 16, 16), 16)
            v = tok[b, r, :].astype(jnp.float32)
            scale = lax.rsqrt(jnp.mean(v * v, axis=-1, keepdims=True) + 1e-06)
            n = (v * scale * gain_ref[...]).astype(jnp.bfloat16)
            to = pl.ds(pl.multiple_of(b * TT + i * 16, 16), 16)
            for s in range(N_FS):
                normed[s, to, :] = n[:, s * 128 : (s + 1) * 128]

    def lhs(step, r):
        return jnp.concatenate([normed[shard[s], r, :] for s in step], axis=1)

    def times(left, step, tile):
        def part(s):
            at = shard[s]
            if tile < 10:
                lo = (tile % 5) * 128
                cuts = [(tile // 5, lo, lo + 128), (tile // 5, F + lo, F + lo + 128)]
            else:
                cuts = [(c, lo, lo + F - FM) for lo in (FM, F + FM) for c in range(2)]
            return jnp.concatenate([wgu[at, c, lo:hi, :] for c, lo, hi in cuts], axis=0)

        right = jnp.concatenate([part(s) for s in step], axis=1)
        return lax.dot_general(left, right, (((1,), (1,)), ((), ())), preferred_element_type=jnp.float32)

    def accumulate(i, part):
        step = steps[i]
        if part > 0:
            need_passed("g", step)
        tiles = (range(0, 5), range(5, 10), range(10, 11))[part]

        @pl.loop(0, 2)
        def _(h):
            r = pl.ds(pl.multiple_of(h * 512, 512), 512)
            left = lhs(step, r)
            for tile in tiles:
                prod = times(left, step, tile)
                if i == 0:
                    acc[tile, r, :] = prod
                else:
                    acc[tile, r, :] += prod

    def gated(g, u):
        return (g / (1.0 + jnp.exp(-g)) * u).astype(jnp.bfloat16)

    def finish(b):
        need_passed("g", steps[-1])
        r = pl.ds(b * TT, TT)
        left = lhs(steps[-1], r)
        for tile in range(11):
            v = acc[tile, r, :] + times(left, steps[-1], tile)
            a, c = v[:, :128], v[:, 128:]
            hid[r, tile * 128 : tile * 128 + 128] = gated(a, c)

    starts = [sum(len(g) for g in groups[:i]) for i in range(len(groups))]

    def half(ref, i, h):
        return ref.at[pl.ds(starts[i], len(groups[i])), pl.ds(h * 128, 128), :]

    def x_copy(kind, i, h):
        src, dst, link = {
            ("far", 0): (far_s, far_r, "x+"), ("far", 1): (far_s, far_r, "x-"),
            ("m", 0): (near_m, in_m, "x-"), ("m", 1): (near_p, in_m, "x+"),
            ("n", 0): (near_p, in_n, "x+"), ("n", 1): (near_m, in_n, "x-"),
        }[(kind, h)]
        c = ("far", "m", "n").index(kind)
        return pltpu.make_async_remote_copy(
            src_ref=half(src, i, h), dst_ref=half(dst, i, h), send_sem=send_sem.at[4 + c],
            recv_sem=x_recv.at[(c * 9 + i) * 2 + h], device_id=peers[link], device_id_type=pl.DeviceIdType.MESH)

    def x_wait(kind, i, h):
        dst = {"far": far_r, "m": in_m, "n": in_n}[kind]
        c = ("far", "m", "n").index(kind)
        ref = half(dst, i, h)
        pltpu.make_async_copy(ref, ref, x_recv.at[(c * 9 + i) * 2 + h]).wait()

    def down(i, b):
        need_passed("d", groups[i])

        def part(s):
            w = [(c, lo, hi) for lo, hi in ((0, FM), (FM, F)) for c in range(2)]
            return jnp.concatenate([wdn[shard[s], c, lo:hi, :] for c, lo, hi in w], axis=0)

        right = [part(s) for s in groups[i]]
        right = right[0] if len(right) == 1 else jnp.concatenate(right, axis=1)
        blocks = range(4) if b is None else (b,)
        r = slice(None) if b is None else pl.ds(b * TT, TT)
        prod = jnp.dot(hid[r, :], right, preferred_element_type=jnp.float32)
        for n, blk in enumerate(blocks):
            to = (far_s, near_p, near_m, own)[blk]
            for j in range(len(groups[i])):
                to[starts[i] + j, :, :] = prod[n * TT : n * TT + TT, j * 128 : j * 128 + 128].astype(to.dtype)
            for kind, h in ((("far", 0), ("far", 1)), (("m", 1),), (("m", 0),), ())[blk]:
                x_copy(kind, i, h).start()

    def add_far(i):
        for h in range(2):
            x_wait("far", i, h)
            ref = (near_p, near_m)[h]
            at = (pl.ds(starts[i], len(groups[i])), pl.ds(h * 128, 128), slice(None))
            ref[at] = (ref[at].astype(jnp.float32) + far_r[at].astype(jnp.float32)).astype(jnp.bfloat16)
            x_copy("n", i, h).start()

    for op, *a in plan:
        if op == "send":
            copy_piece(*a).start()
        elif op == "recv":
            recv_piece(*a)
        elif op == "pass":
            pass_shard(*a)
        elif op == "norm":
            norm(*a)
        elif op == "acc":
            accumulate(*a)
        elif op == "fin":
            finish(*a)
        elif op == "add":
            add_far(*a)
        else:
            down(*a)

    f32 = jnp.float32
    for i in range(len(groups)):
        for h in range(2):
            x_wait("m", i, h)
            x_wait("n", i, h)
        for j, s in enumerate(groups[i]):
            u = starts[i] + j
            total = own[u] + in_m[u].astype(f32) + in_n[u].astype(f32)
            out_ref[:, pl.ds(pl.multiple_of(shard[s] * 128, 128), 128)] = total.astype(jnp.bfloat16)

    sent = (wgu.at[pl.ds(0, 15), 0], wdn.at[pl.ds(0, 15), 0], wgu.at[:, 0], wdn.at[:, 0], far_s, near_p, near_m)
    for i, ref in enumerate(sent):
        pltpu.make_async_copy(ref, ref, send_sem.at[i]).wait()


def per_device(tokens, norm_gain, gate_weight, up_weight, down_weight):
    vmem, dma = pltpu.VMEM, pltpu.SemaphoreType.DMA
    bf, f32 = jnp.bfloat16, jnp.float32
    unit = (N_FS, TT, 128)
    args = (tokens, norm_gain.reshape(1, D), gate_weight.T, up_weight.T, down_weight)
    any_spec = pl.BlockSpec(memory_space=pltpu.HBM)
    return pl.pallas_call(
        kernel,
        out_shape=jax.ShapeDtypeStruct((TT, D), bf),
        in_specs=[any_spec, pl.BlockSpec(memory_space=pltpu.VMEM), any_spec, any_spec, any_spec],
        out_specs=pl.BlockSpec(memory_space=pltpu.VMEM),
        scratch_shapes=[
            vmem((4, TT, D), bf), vmem((N_FS, 4 * TT, 128), bf), vmem((N_FS, 2, 2 * F, 128), bf), vmem((N_FS, 2, F, 128), bf),
            vmem((11, 4 * TT, 256), f32), vmem((4 * TT, 2 * F), bf),
            vmem(unit, bf), vmem(unit, bf), vmem(unit, bf), vmem(unit, bf), vmem(unit, bf), vmem(unit, bf), vmem(unit, f32),
            dma((3,)), dma((4,)), dma((64,)), dma((64,)), dma((16,)), dma((16,)), dma((54,)), dma((7,)),
        ],
        compiler_params=pltpu.CompilerParams(collective_id=0, has_side_effects=True, vmem_limit_bytes=52 * 2**20),
        name="ffn",
    )(*(pltpu.with_memory_space_constraint(a, pltpu.HBM) for a in args))


def solution(mesh):
    placed = (P("fs", None), P(), P("fs", "tp"), P("fs", "tp"), P("tp", "fs"))
    return jax.shard_map(
        per_device, mesh=mesh, in_specs=placed, out_specs=P(("fs", "tp"), None), check_vma=False
    )
```

```python
import heapq

import jax
import jax.numpy as jnp
from jax import lax
from jax.experimental import pallas as pl
from jax.experimental.pallas import tpu as pltpu
from jax.sharding import PartitionSpec as P

D = 2048
N_FS = 16
F = 704
FM = 640
TT = 256
GQ = 352
DQ = 176
RANK = {1: 1, 2: 2, 4: 3, 5: 4, 8: 5}
LINKS = ("y+", "y-", "z+", "z-")
FIRST = {"y+": (0, 1, 2, 3), "y-": (1, 0, 3, 2), "z+": (2, 3, 0, 1), "z-": (3, 2, 1, 0)}


def near(d):
    return (d + 1) % 4 - 1


def onward(q, dz, dy):
    first, second = ("y", "z") if q < 2 else ("z", "y")
    sign = "+" if q % 2 == 0 else "-"
    a, b = (dy, dz) if q < 2 else (dz, dy)
    came = {-1: "+", 1: "-"}
    if b == 0:
        out = [first + sign] if came.get(a) == sign else []
        return out + [second + sign, second + ("-" if sign == "+" else "+")]
    return [second + sign] if came.get(b) == sign else []


def seen_from(link, dz, dy):
    step = 1 if link[1] == "+" else -1
    return (near(dz - step), dy) if link[0] == "z" else (dz, near(dy - step))


def turn(q, dz, dy):
    a, b = (dy, dz) if q < 2 else (dz, dy)
    sign = 1 - 2 * (q % 2)
    return (near(sign * a) + 1) * 4 + near(sign * b) + 1


def gather_events(unit, lat, backlog):
    free = {l: 0.0 for l in LINKS}
    count = {l: 0 for l in LINKS}
    heap = {l: [] for l in LINKS}
    flying, n = [], 0

    def offer(l, k, q, dz, dy):
        nonlocal n
        n += 1
        tz, ty = seen_from(l, dz, dy)
        early = tz == 0 if q < 2 else ty == 0
        heapq.heappush(heap[l], (k == "d", 0 if early else RANK[tz * tz + ty * ty], n, k, q, dz, dy))

    def top_up(t):
        nonlocal n
        sends = []
        for l in LINKS:
            while heap[l] and free[l] - t < backlog and (heap[l][0][0] == 0 or count[l] >= 15):
                _, _, _, k, q, dz, dy = heapq.heappop(heap[l])
                count[l] += 1
                n += 1
                free[l] = max(t, free[l]) + unit[k]
                sends.append((l, k, q, dz, dy))
                heapq.heappush(flying, (free[l] + lat, n, k, q, *seen_from(l, dz, dy)))
        return sends

    for l in LINKS:
        for k in "gd":
            for q in FIRST[l]:
                offer(l, k, q, 0, 0)
    events = [(0.0, None, top_up(0.0))]
    here = {}
    while flying:
        t, _, k, q, dz, dy = heapq.heappop(flying)
        some = here.setdefault((k, turn(q, dz, dy)), [])
        some.append((q, dz, dy))
        if len(some) == 4:
            for piece in some:
                for l in onward(*piece):
                    offer(l, k, *piece)
            events.append((t, (k, turn(q, dz, dy), some), top_up(t)))
    assert len(events) == 31
    return events


def make_plan(unit={"g": 1.93, "d": 0.97}, lat=2.2, backlog=6.0, sib=1.8, sizes=(5, 6, 2, 3), margin=0.4, log=None):
    events = gather_events(unit, lat, backlog)
    done, left = {("g", 0, 0): 0.0, ("d", 0, 0): 0.0}, {}
    for t, what, _ in events[1:]:
        for _, dz, dy in what[2]:
            key = (what[0], dz, dy)
            left[key] = left.get(key, 0) + 1
            if left[key] == 4:
                done[key] = t + margin
    order = {k: [key[1:] for key in sorted((key for key in done if key[0] == k), key=lambda key: done[key])] for k in "gd"}
    assert len(order["g"]) == 16 and len(order["d"]) == 16
    steps = [order["g"][sum(sizes[:i]) : sum(sizes[: i + 1])] for i in range(len(sizes))]
    groups = [order["d"][:1]] + [order["d"][1 + 2 * i : 3 + 2 * i] for i in range(7)] + [order["d"][15:]]
    last = len(steps) - 1
    work = [(0.0, 1.9, ("norm", b)) for b in range(4)]
    for i in range(last):
        ready = max(done[("g", *s)] for s in steps[i])
        cost = 0.43 * len(steps[i])
        work.append((ready, cost, ("acc", i, 0)))
        work.append((ready + sib, cost, ("acc", i, 1)))
        work.append((ready + sib, cost * 0.35, ("acc", i, 2)))
    cost = 0.45 + 0.15 * len(steps[last])
    ready = max(done[("g", *s)] for s in steps[last])
    late = max(done[("d", *s)] for s in groups[1]) + sib
    for b in range(4):
        work += [(ready, cost, ("fin", b)), (ready, 0.38, ("down", 0, b))]
    work[-1:] = [(late, 0.55, ("down", 1, b)) for b in range(3)] + work[-1:] + [(late, 0.55, ("down", 1, 3))]
    for i in range(2, len(groups)):
        ready = max(done[("d", *s)] for s in groups[i]) + sib
        work.append((ready, 1.8, ("down", i, None)))
        if i == 2:
            work.append((ready, 0.1, ("add", 0)))
    work += [(60.0, 0.1, ("add", i)) for i in range(1, len(groups))]
    plan, now, got, events = [], 0.0, {}, events[::-1]
    plan += [("send", *s) for s in events.pop()[2]] + [("pass", "g", 0, 0), ("pass", "d", 0, 0)]
    while events or work:
        free = [item for item in work if item[0] <= now]
        soon = min([item[0] for item in work], default=1e9)
        if events and events[-1][0] + margin <= (now if free else soon):
            t, what, sends = events.pop()
            plan.append(("recv", *what[:2]))
            now = max(now, t + margin)
            plan += [("send", *s) for s in sends]
            for _, dz, dy in what[2]:
                key = (what[0], dz, dy)
                got[key] = got.get(key, 0) + 1
                if got[key] == 4:
                    plan.append(("pass", *key))
        elif free:
            work.remove(free[0])
            plan.append(free[0][2])
            if log is not None:
                log.append((round(now, 1), free[0][2]))
            now += free[0][1]
        else:
            now = soon
    return plan, steps, groups


def kernel(tok_hbm, gain_hbm, gate_hbm, up_hbm, dn_hbm, out_ref, tok, normed, wgu, wdn, acc, hid, far_s, far_r, near_p, near_m,
           come, own, loc_sem, tok_sem, g_recv, d_recv, gs_recv, ds_recv, x_recv, send_sem, gain_ref):
    plan, steps, groups = make_plan()
    fs, tp = lax.axis_index("fs"), lax.axis_index("tp")
    z, y = fs // 4, fs % 4
    x, core = tp // 2, tp % 2

    def dev(link):
        step = 1 if link[1] == "+" else 3
        if link[0] == "z":
            return {"fs": ((z + step) % 4) * 4 + y, "tp": tp}
        if link[0] == "y":
            return {"fs": z * 4 + (y + step) % 4, "tp": tp}
        if link[0] == "x":
            return {"fs": fs, "tp": ((x + step) % 4) * 2 + core}
        return {"fs": fs, "tp": x * 2 + 1 - core}

    peers = {l: dev(l) for l in LINKS + ("x+", "x-", "c+")}
    shard = {(dz, dy): ((z + dz + 4) % 4) * 4 + (y + dy + 4) % 4 for dz in range(-1, 3) for dy in range(-1, 3)}

    def piece(k, q, dz, dy):
        if k == "g":
            return wgu.at[shard[(dz, dy)], 0, pl.ds(q * GQ, GQ), :]
        return wdn.at[shard[(dz, dy)], 0, pl.ds(q * DQ, DQ), :]

    def copy_piece(link, k, q, dz, dy):
        there = seen_from(link, dz, dy)
        ref = piece(k, q, dz, dy)
        sems, s = (g_recv, 0) if k == "g" else (d_recv, 1)
        return pltpu.make_async_remote_copy(
            src_ref=ref, dst_ref=ref, send_sem=send_sem.at[s], recv_sem=sems.at[turn(q, *there)],
            device_id=peers[link], device_id_type=pl.DeviceIdType.MESH)

    def recv_turn(k, at):
        ref = (wgu if k == "g" else wdn).at[0, 0]
        pltpu.make_async_copy(ref, ref, (g_recv if k == "g" else d_recv).at[at]).wait()

    def whole(k, slot, dz, dy):
        return (wgu if k == "g" else wdn).at[shard[(dz, dy)], slot]

    def batch(k, s):
        return next(i for i, part in enumerate(steps if k == "g" else groups) if s in part)

    def pass_shard(k, dz, dy):
        sems, s = (gs_recv, 2) if k == "g" else (ds_recv, 3)
        pltpu.make_async_remote_copy(
            src_ref=whole(k, 0, dz, dy), dst_ref=whole(k, 1, dz, dy), send_sem=send_sem.at[s],
            recv_sem=sems.at[batch(k, (dz, dy))], device_id=peers["c+"], device_id_type=pl.DeviceIdType.MESH).start()

    passed = set()

    def need_passed(k, shards):
        at = batch(k, shards[0])
        if (k, at) not in passed:
            passed.add((k, at))
            ref = (wgu if k == "g" else wdn).at[pl.ds(0, len(shards)), 1]
            pltpu.make_async_copy(ref, ref, (gs_recv if k == "g" else ds_recv).at[at]).wait()

    barrier = pltpu.get_barrier_semaphore()
    for peer in peers.values():
        pl.semaphore_signal(barrier, inc=1, device_id=peer, device_id_type=pl.DeviceIdType.MESH)
    own_g = pltpu.make_async_copy(gate_hbm, whole("g", 0, 0, 0).at[pl.ds(0, F), :], loc_sem.at[0])
    own_u = pltpu.make_async_copy(up_hbm, whole("g", 0, 0, 0).at[pl.ds(F, F), :], loc_sem.at[1])
    own_d = pltpu.make_async_copy(dn_hbm, whole("d", 0, 0, 0), loc_sem.at[2])
    own_g.start()
    own_u.start()
    own_d.start()
    gain = pltpu.make_async_copy(gain_hbm, gain_ref, loc_sem.at[3])
    gain.start()

    def tok_copy(b):
        to = (x + (2, 1, 3, 0)[b]) % 4
        at = pl.multiple_of((to * 2 + core) * TT, TT)
        return pltpu.make_async_copy(tok_hbm.at[pl.ds(at, TT), :], tok.at[b], tok_sem.at[b])

    own_g.wait()
    own_u.wait()
    own_d.wait()
    gain.wait()
    for b in range(4):
        tok_copy(b).start()
    pl.semaphore_wait(barrier, len(peers))

    def norm(b):
        tok_copy(b).wait()

        @pl.loop(0, TT // 16)
        def _(i):
            r = pl.ds(pl.multiple_of(i * 16, 16), 16)
            v = tok[b, r, :].astype(jnp.float32)
            scale = lax.rsqrt(jnp.mean(v * v, axis=-1, keepdims=True) + 1e-06)
            n = (v * scale * gain_ref[...]).astype(jnp.bfloat16)
            to = pl.ds(pl.multiple_of(b * TT + i * 16, 16), 16)
            for s in range(N_FS):
                normed[s, to, :] = n[:, s * 128 : (s + 1) * 128]

    def lhs(step, r):
        return jnp.concatenate([normed[shard[s], r, :] for s in step], axis=1)

    def times(left, step, tile):
        def part(s):
            at = shard[s]
            if tile < 10:
                lo = (tile % 5) * 128
                cuts = [(tile // 5, lo, lo + 128), (tile // 5, F + lo, F + lo + 128)]
            else:
                cuts = [(c, lo, lo + F - FM) for lo in (FM, F + FM) for c in range(2)]
            return jnp.concatenate([wgu[at, c, lo:hi, :] for c, lo, hi in cuts], axis=0)

        right = jnp.concatenate([part(s) for s in step], axis=1)
        return lax.dot_general(left, right, (((1,), (1,)), ((), ())), preferred_element_type=jnp.float32)

    def accumulate(i, part):
        step = steps[i]
        if part > 0:
            need_passed("g", step)
        tiles = (range(0, 5), range(5, 10), range(10, 11))[part]

        @pl.loop(0, 2)
        def _(h):
            r = pl.ds(pl.multiple_of(h * 512, 512), 512)
            left = lhs(step, r)
            for tile in tiles:
                prod = times(left, step, tile)
                if i == 0:
                    acc[tile, r, :] = prod
                else:
                    acc[tile, r, :] += prod

    def gated(g, u):
        return (g / (1.0 + jnp.exp(-g)) * u).astype(jnp.bfloat16)

    def finish(b):
        r = pl.ds(b * TT, TT)
        left = lhs(steps[-1], r)
        for tile in range(11):
            if tile == 5:
                need_passed("g", steps[-1])
            v = acc[tile, r, :] + times(left, steps[-1], tile)
            a, c = v[:, :128], v[:, 128:]
            hid[r, tile * 128 : tile * 128 + 128] = gated(a, c)

    starts = [sum(len(g) for g in groups[:i]) for i in range(len(groups))]

    def half(ref, i, h):
        return ref.at[pl.ds(starts[i], len(groups[i])), pl.ds(h * 128, 128), :]

    def x_copy(kind, i, h):
        src, dst, link = {
            ("far", 0): (far_s, far_r, "x+"), ("far", 1): (far_s, far_r, "x-"),
            ("m", 0): (near_m, come.at[0], "x-"), ("m", 1): (near_p, come.at[0], "x+"),
            ("n", 0): (near_p, come.at[1], "x+"), ("n", 1): (near_m, come.at[1], "x-"),
        }[(kind, h)]
        c = ("far", "m", "n").index(kind)
        return pltpu.make_async_remote_copy(
            src_ref=half(src, i, h), dst_ref=half(dst, i, h), send_sem=send_sem.at[4 + c],
            recv_sem=x_recv.at[i if kind == "far" else 9 + i], device_id=peers[link], device_id_type=pl.DeviceIdType.MESH)

    def x_wait(ref, i, at):
        pltpu.make_async_copy(ref, ref, x_recv.at[at]).wait()

    def down(i, b):
        need_passed("d", groups[i])

        def part(s):
            w = [(c, lo, hi) for lo, hi in ((0, FM), (FM, F)) for c in range(2)]
            return jnp.concatenate([wdn[shard[s], c, lo:hi, :] for c, lo, hi in w], axis=0)

        right = [part(s) for s in groups[i]]
        right = right[0] if len(right) == 1 else jnp.concatenate(right, axis=1)
        blocks = range(4) if b is None else (b,)
        r = slice(None) if b is None else pl.ds(b * TT, TT)
        prod = jnp.dot(hid[r, :], right, preferred_element_type=jnp.float32)
        for n, blk in enumerate(blocks):
            to = (far_s, near_p, near_m, own)[blk]
            for j in range(len(groups[i])):
                to[starts[i] + j, :, :] = prod[n * TT : n * TT + TT, j * 128 : j * 128 + 128].astype(to.dtype)
            for kind, h in ((("far", 0), ("far", 1)), (("m", 1),), (("m", 0),), ())[blk]:
                x_copy(kind, i, h).start()

    def add_far(i):
        units = pl.ds(starts[i], len(groups[i]))
        x_wait(far_r.at[units], i, i)
        for h in range(2):
            ref = (near_p, near_m)[h]
            at = (units, pl.ds(h * 128, 128), slice(None))
            ref[at] = (ref[at].astype(jnp.float32) + far_r[at].astype(jnp.float32)).astype(jnp.bfloat16)
            x_copy("n", i, h).start()

    for op, *a in plan:
        if op == "send":
            copy_piece(*a).start()
        elif op == "recv":
            recv_turn(*a)
        elif op == "pass":
            pass_shard(*a)
        elif op == "norm":
            norm(*a)
        elif op == "acc":
            accumulate(*a)
        elif op == "fin":
            finish(*a)
        elif op == "add":
            add_far(*a)
        else:
            down(*a)

    f32 = jnp.float32
    for i in range(len(groups)):
        x_wait(come.at[:, pl.ds(starts[i], len(groups[i]))], i, 9 + i)
        for j, s in enumerate(groups[i]):
            u = starts[i] + j
            cols = pl.ds(pl.multiple_of(shard[s] * 128, 128), 128)
            total = own[u] + come[0, u].astype(f32) + come[1, u].astype(f32)
            out_ref[:, cols] = total.astype(jnp.bfloat16)

    sent = (wgu.at[pl.ds(0, 15), 0], wdn.at[pl.ds(0, 15), 0], wgu.at[:, 0], wdn.at[:, 0], far_s, near_p, near_m)
    for i, ref in enumerate(sent):
        pltpu.make_async_copy(ref, ref, send_sem.at[i]).wait()


def per_device(tokens, norm_gain, gate_weight, up_weight, down_weight):
    vmem, dma = pltpu.VMEM, pltpu.SemaphoreType.DMA
    bf, f32 = jnp.bfloat16, jnp.float32
    unit = (N_FS, TT, 128)
    args = (tokens, norm_gain.reshape(1, D), gate_weight.T, up_weight.T, down_weight)
    any_spec = pl.BlockSpec(memory_space=pltpu.HBM)
    return pl.pallas_call(
        kernel,
        out_shape=jax.ShapeDtypeStruct((TT, D), bf),
        in_specs=[any_spec] * 5,
        out_specs=pl.BlockSpec(memory_space=pltpu.VMEM),
        scratch_shapes=[
            vmem((4, TT, D), bf), vmem((N_FS, 4 * TT, 128), bf), vmem((N_FS, 2, 2 * F, 128), bf), vmem((N_FS, 2, F, 128), bf),
            vmem((11, 4 * TT, 256), f32), vmem((4 * TT, 2 * F), bf),
            vmem(unit, bf), vmem(unit, bf), vmem(unit, bf), vmem(unit, bf), vmem((2, *unit), bf), vmem(unit, f32),
            dma((4,)), dma((4,)), dma((16,)), dma((16,)), dma((4,)), dma((9,)), dma((18,)), dma((7,)), vmem((1, D), f32),
        ],
        compiler_params=pltpu.CompilerParams(collective_id=0, has_side_effects=True, vmem_limit_bytes=52 * 2**20),
        name="ffn",
    )(*(pltpu.with_memory_space_constraint(a, pltpu.HBM) for a in args))


def solution(mesh):
    placed = (P("fs", None), P(), P("fs", "tp"), P("fs", "tp"), P("tp", "fs"))
    return jax.shard_map(
        per_device, mesh=mesh, in_specs=placed, out_specs=P(("fs", "tp"), None), check_vma=False
    )
```

```python
import heapq

import jax
import jax.numpy as jnp
from jax import lax
from jax.experimental import pallas as pl
from jax.experimental.pallas import tpu as pltpu
from jax.sharding import PartitionSpec as P

D = 2048
N_FS = 16
F = 704
FM = 640
TT = 256
GQ = 352
DQ = 176
RANK = {1: 1, 2: 2, 4: 3, 5: 4, 8: 5}
LINKS = ("y+", "y-", "z+", "z-")
FIRST = {"y+": (0, 1, 2, 3), "y-": (1, 0, 3, 2), "z+": (2, 3, 0, 1), "z-": (3, 2, 1, 0)}


def near(d):
    return (d + 1) % 4 - 1


def onward(q, dz, dy):
    first, second = ("y", "z") if q < 2 else ("z", "y")
    sign = "+" if q % 2 == 0 else "-"
    a, b = (dy, dz) if q < 2 else (dz, dy)
    came = {-1: "+", 1: "-"}
    if b == 0:
        out = [first + sign] if came.get(a) == sign else []
        return out + [second + sign, second + ("-" if sign == "+" else "+")]
    return [second + sign] if came.get(b) == sign else []


def seen_from(link, dz, dy):
    step = 1 if link[1] == "+" else -1
    return (near(dz - step), dy) if link[0] == "z" else (dz, near(dy - step))


def turn(q, dz, dy):
    a, b = (dy, dz) if q < 2 else (dz, dy)
    sign = 1 - 2 * (q % 2)
    return (near(sign * a) + 1) * 4 + near(sign * b) + 1


def gather_events(unit, lat, backlog):
    free = {l: 0.0 for l in LINKS}
    count = {l: 0 for l in LINKS}
    heap = {l: [] for l in LINKS}
    flying, n = [], 0

    def offer(l, k, q, dz, dy):
        nonlocal n
        n += 1
        tz, ty = seen_from(l, dz, dy)
        early = tz == 0 if q < 2 else ty == 0
        heapq.heappush(heap[l], (k == "d", 0 if early else RANK[tz * tz + ty * ty], n, k, q, dz, dy))

    def top_up(t):
        nonlocal n
        sends = []
        for l in LINKS:
            while heap[l] and free[l] - t < backlog and (heap[l][0][0] == 0 or count[l] >= 15):
                _, _, _, k, q, dz, dy = heapq.heappop(heap[l])
                count[l] += 1
                n += 1
                free[l] = max(t, free[l]) + unit[k]
                sends.append((l, k, q, dz, dy))
                heapq.heappush(flying, (free[l] + lat, n, k, q, *seen_from(l, dz, dy)))
        return sends

    for l in LINKS:
        for k in "gd":
            for q in FIRST[l]:
                offer(l, k, q, 0, 0)
    events = [(0.0, None, top_up(0.0))]
    here = {}
    while flying:
        t, _, k, q, dz, dy = heapq.heappop(flying)
        some = here.setdefault((k, turn(q, dz, dy)), [])
        some.append((q, dz, dy))
        if len(some) == 4:
            for piece in some:
                for l in onward(*piece):
                    offer(l, k, *piece)
            events.append((t, (k, turn(q, dz, dy), some), top_up(t)))
    assert len(events) == 31
    return events


def make_plan(unit={"g": 1.93, "d": 0.97}, lat=2.2, backlog=6.0, sib=1.8, sizes=(5, 6, 2, 3), margin=0.4, ahead=1.2, log=None):
    events = gather_events(unit, lat, backlog)
    done, left = {("g", 0, 0): 0.0, ("d", 0, 0): 0.0}, {}
    for t, what, _ in events[1:]:
        for _, dz, dy in what[2]:
            key = (what[0], dz, dy)
            left[key] = left.get(key, 0) + 1
            if left[key] == 4:
                done[key] = t + margin
    order = {k: [key[1:] for key in sorted((key for key in done if key[0] == k), key=lambda key: done[key])] for k in "gd"}
    assert len(order["g"]) == 16 and len(order["d"]) == 16
    steps = [order["g"][sum(sizes[:i]) : sum(sizes[: i + 1])] for i in range(len(sizes))]
    groups = [order["d"][:1]] + [order["d"][1 + 2 * i : 3 + 2 * i] for i in range(7)] + [order["d"][15:]]
    last = len(steps) - 1
    work = [(0.0, 1.9, ("norm", b)) for b in range(4)]
    for i in range(last):
        ready = max(done[("g", *s)] for s in steps[i])
        cost = 0.43 * len(steps[i])
        work.append((ready, cost, ("acc", i, 0)))
        work.append((ready + sib, cost, ("acc", i, 1)))
        work.append((ready + sib, cost * 0.35, ("acc", i, 2)))
    cost = 0.45 + 0.15 * len(steps[last])
    ready = max(done[("g", *s)] for s in steps[last])
    late = max(done[("d", *s)] for s in groups[1]) + 0.3
    for b in range(4):
        work += [(ready, cost, ("fin", b)), (ready, 0.38, ("down", 0, b))]
    work[-1:] = [(late, 0.55, ("down", 1, b)) for b in range(3)] + work[-1:] + [(late, 0.55, ("down", 1, 3))]
    for i in range(2, len(groups)):
        ready = max(done[("d", *s)] for s in groups[i]) + sib
        work.append((ready, 1.8, ("down", i, None)))
        if i == 2:
            work.append((ready, 0.1, ("add", 0)))
    work += [(60.0, 0.1, ("add", i)) for i in range(1, len(groups))]
    first_due = {("d", *s) for s in groups[1]}
    plan, now, got, events = [], 0.0, {}, events[::-1]
    plan += [("send", *s) for s in events.pop()[2]] + [("pass", "g", 0, 0), ("pass", "d", 0, 0)]
    while events or work:
        free = [item for item in work if item[0] <= now]
        soon = min([item[0] for item in work], default=1e9)
        urgent = events and any((events[-1][1][0], *p[1:]) in first_due and got.get(("d", *p[1:]), 0) == 3 for p in events[-1][1][2])
        if events and events[-1][0] + margin <= (now if free else soon) + (ahead if urgent else 0.0):
            t, what, sends = events.pop()
            plan.append(("recv", *what[:2]))
            now = max(now, t + margin)
            plan += [("send", *s) for s in sends]
            for _, dz, dy in what[2]:
                key = (what[0], dz, dy)
                got[key] = got.get(key, 0) + 1
                if got[key] == 4:
                    plan.append(("pass", *key))
        elif free:
            work.remove(free[0])
            plan.append(free[0][2])
            if log is not None:
                log.append((round(now, 1), free[0][2]))
            now += free[0][1]
        else:
            now = soon
    return plan, steps, groups


def kernel(tok_hbm, gain_hbm, gate_hbm, up_hbm, dn_hbm, out_ref, tok, normed, wgu, wdn, acc, hid, far_s, far_r, near_p, near_m,
           come, own, loc_sem, tok_sem, g_recv, d_recv, gs_recv, ds_recv, x_recv, send_sem, gain_ref):
    plan, steps, groups = make_plan()
    fs, tp = lax.axis_index("fs"), lax.axis_index("tp")
    z, y = fs // 4, fs % 4
    x, core = tp // 2, tp % 2

    def dev(link):
        step = 1 if link[1] == "+" else 3
        if link[0] == "z":
            return {"fs": ((z + step) % 4) * 4 + y, "tp": tp}
        if link[0] == "y":
            return {"fs": z * 4 + (y + step) % 4, "tp": tp}
        if link[0] == "x":
            return {"fs": fs, "tp": ((x + step) % 4) * 2 + core}
        return {"fs": fs, "tp": x * 2 + 1 - core}

    peers = {l: dev(l) for l in LINKS + ("x+", "x-", "c+")}
    shard = {(dz, dy): ((z + dz + 4) % 4) * 4 + (y + dy + 4) % 4 for dz in range(-1, 3) for dy in range(-1, 3)}

    def piece(k, q, dz, dy):
        if k == "g":
            return wgu.at[shard[(dz, dy)], 0, pl.ds(q * GQ, GQ), :]
        return wdn.at[shard[(dz, dy)], 0, pl.ds(q * DQ, DQ), :]

    def copy_piece(link, k, q, dz, dy):
        there = seen_from(link, dz, dy)
        ref = piece(k, q, dz, dy)
        sems, s = (g_recv, 0) if k == "g" else (d_recv, 1)
        return pltpu.make_async_remote_copy(
            src_ref=ref, dst_ref=ref, send_sem=send_sem.at[s], recv_sem=sems.at[turn(q, *there)],
            device_id=peers[link], device_id_type=pl.DeviceIdType.MESH)

    def recv_turn(k, at):
        ref = (wgu if k == "g" else wdn).at[0, 0]
        pltpu.make_async_copy(ref, ref, (g_recv if k == "g" else d_recv).at[at]).wait()

    def whole(k, slot, dz, dy):
        return (wgu if k == "g" else wdn).at[shard[(dz, dy)], slot]

    def batch(k, s):
        return next(i for i, part in enumerate(steps if k == "g" else groups) if s in part)

    def pass_shard(k, dz, dy):
        sems, s = (gs_recv, 2) if k == "g" else (ds_recv, 3)
        pltpu.make_async_remote_copy(
            src_ref=whole(k, 0, dz, dy), dst_ref=whole(k, 1, dz, dy), send_sem=send_sem.at[s],
            recv_sem=sems.at[batch(k, (dz, dy))], device_id=peers["c+"], device_id_type=pl.DeviceIdType.MESH).start()

    passed = set()

    def need_passed(k, shards):
        at = batch(k, shards[0])
        if (k, at) not in passed:
            passed.add((k, at))
            ref = (wgu if k == "g" else wdn).at[pl.ds(0, len(shards)), 1]
            pltpu.make_async_copy(ref, ref, (gs_recv if k == "g" else ds_recv).at[at]).wait()

    barrier = pltpu.get_barrier_semaphore()
    for peer in peers.values():
        pl.semaphore_signal(barrier, inc=1, device_id=peer, device_id_type=pl.DeviceIdType.MESH)
    own_g = pltpu.make_async_copy(gate_hbm, whole("g", 0, 0, 0).at[pl.ds(0, F), :], loc_sem.at[0])
    own_u = pltpu.make_async_copy(up_hbm, whole("g", 0, 0, 0).at[pl.ds(F, F), :], loc_sem.at[1])
    own_d = pltpu.make_async_copy(dn_hbm, whole("d", 0, 0, 0), loc_sem.at[2])
    own_g.start()
    own_u.start()
    own_d.start()
    gain = pltpu.make_async_copy(gain_hbm, gain_ref, loc_sem.at[3])
    gain.start()

    def tok_copy(b):
        to = (x + (2, 1, 3, 0)[b]) % 4
        at = pl.multiple_of((to * 2 + core) * TT, TT)
        return pltpu.make_async_copy(tok_hbm.at[pl.ds(at, TT), :], tok.at[b], tok_sem.at[b])

    own_g.wait()
    own_u.wait()
    own_d.wait()
    gain.wait()
    for b in range(4):
        tok_copy(b).start()
    pl.semaphore_wait(barrier, len(peers))

    def norm(b):
        tok_copy(b).wait()

        @pl.loop(0, TT // 16)
        def _(i):
            r = pl.ds(pl.multiple_of(i * 16, 16), 16)
            v = tok[b, r, :].astype(jnp.float32)
            scale = lax.rsqrt(jnp.mean(v * v, axis=-1, keepdims=True) + 1e-06)
            n = (v * scale * gain_ref[...]).astype(jnp.bfloat16)
            to = pl.ds(pl.multiple_of(b * TT + i * 16, 16), 16)
            for s in range(N_FS):
                normed[s, to, :] = n[:, s * 128 : (s + 1) * 128]

    def lhs(step, r):
        return jnp.concatenate([normed[shard[s], r, :] for s in step], axis=1)

    def times(left, step, tile):
        def part(s):
            at = shard[s]
            if tile < 10:
                lo = (tile % 5) * 128
                cuts = [(tile // 5, lo, lo + 128), (tile // 5, F + lo, F + lo + 128)]
            else:
                cuts = [(c, lo, lo + F - FM) for lo in (FM, F + FM) for c in range(2)]
            return jnp.concatenate([wgu[at, c, lo:hi, :] for c, lo, hi in cuts], axis=0)

        right = jnp.concatenate([part(s) for s in step], axis=1)
        return lax.dot_general(left, right, (((1,), (1,)), ((), ())), preferred_element_type=jnp.float32)

    def accumulate(i, part):
        step = steps[i]
        if part > 0:
            need_passed("g", step)
        tiles = (range(0, 5), range(5, 10), range(10, 11))[part]

        @pl.loop(0, 2)
        def _(h):
            r = pl.ds(pl.multiple_of(h * 512, 512), 512)
            left = lhs(step, r)
            for tile in tiles:
                prod = times(left, step, tile)
                if i == 0:
                    acc[tile, r, :] = prod
                else:
                    acc[tile, r, :] += prod

    def gated(g, u):
        return (g / (1.0 + jnp.exp(-g)) * u).astype(jnp.bfloat16)

    def finish(b):
        r = pl.ds(b * TT, TT)
        left = lhs(steps[-1], r)
        for tile in range(11):
            if tile == 5:
                need_passed("g", steps[-1])
            v = acc[tile, r, :] + times(left, steps[-1], tile)
            a, c = v[:, :128], v[:, 128:]
            hid[r, tile * 128 : tile * 128 + 128] = gated(a, c)

    starts = [sum(len(g) for g in groups[:i]) for i in range(len(groups))]

    def half(ref, i, h):
        return ref.at[pl.ds(starts[i], len(groups[i])), pl.ds(h * 128, 128), :]

    def x_copy(kind, i, h):
        src, dst, link = {
            ("far", 0): (far_s, far_r, "x+"), ("far", 1): (far_s, far_r, "x-"),
            ("m", 0): (near_m, come.at[0], "x-"), ("m", 1): (near_p, come.at[0], "x+"),
            ("n", 0): (near_p, come.at[1], "x+"), ("n", 1): (near_m, come.at[1], "x-"),
        }[(kind, h)]
        c = ("far", "m", "n").index(kind)
        return pltpu.make_async_remote_copy(
            src_ref=half(src, i, h), dst_ref=half(dst, i, h), send_sem=send_sem.at[4 + c],
            recv_sem=x_recv.at[i if kind == "far" else 9 + i], device_id=peers[link], device_id_type=pl.DeviceIdType.MESH)

    def x_wait(ref, i, at):
        pltpu.make_async_copy(ref, ref, x_recv.at[at]).wait()

    def down(i, b):
        need_passed("d", groups[i])

        def part(s):
            w = [(c, lo, hi) for lo, hi in ((0, FM), (FM, F)) for c in range(2)]
            return jnp.concatenate([wdn[shard[s], c, lo:hi, :] for c, lo, hi in w], axis=0)

        right = [part(s) for s in groups[i]]
        right = right[0] if len(right) == 1 else jnp.concatenate(right, axis=1)
        blocks = range(4) if b is None else (b,)
        r = slice(None) if b is None else pl.ds(b * TT, TT)
        prod = jnp.dot(hid[r, :], right, preferred_element_type=jnp.float32)
        for n, blk in enumerate(blocks):
            to = (far_s, near_p, near_m, own)[blk]
            for j in range(len(groups[i])):
                to[starts[i] + j, :, :] = prod[n * TT : n * TT + TT, j * 128 : j * 128 + 128].astype(to.dtype)
            for kind, h in ((("far", 0), ("far", 1)), (("m", 1),), (("m", 0),), ())[blk]:
                x_copy(kind, i, h).start()

    def add_far(i):
        units = pl.ds(starts[i], len(groups[i]))
        x_wait(far_r.at[units], i, i)
        for h in range(2):
            ref = (near_p, near_m)[h]
            at = (units, pl.ds(h * 128, 128), slice(None))
            ref[at] = (ref[at].astype(jnp.float32) + far_r[at].astype(jnp.float32)).astype(jnp.bfloat16)
            x_copy("n", i, h).start()

    for op, *a in plan:
        if op == "send":
            copy_piece(*a).start()
        elif op == "recv":
            recv_turn(*a)
        elif op == "pass":
            pass_shard(*a)
        elif op == "norm":
            norm(*a)
        elif op == "acc":
            accumulate(*a)
        elif op == "fin":
            finish(*a)
        elif op == "add":
            add_far(*a)
        else:
            down(*a)

    f32 = jnp.float32
    for i in range(len(groups)):
        x_wait(come.at[:, pl.ds(starts[i], len(groups[i]))], i, 9 + i)
        for j, s in enumerate(groups[i]):
            u = starts[i] + j
            cols = pl.ds(pl.multiple_of(shard[s] * 128, 128), 128)
            total = own[u] + come[0, u].astype(f32) + come[1, u].astype(f32)
            out_ref[:, cols] = total.astype(jnp.bfloat16)

    sent = (wgu.at[pl.ds(0, 15), 0], wdn.at[pl.ds(0, 15), 0], wgu.at[:, 0], wdn.at[:, 0], far_s, near_p, near_m)
    for i, ref in enumerate(sent):
        pltpu.make_async_copy(ref, ref, send_sem.at[i]).wait()


def per_device(tokens, norm_gain, gate_weight, up_weight, down_weight):
    vmem, dma = pltpu.VMEM, pltpu.SemaphoreType.DMA
    bf, f32 = jnp.bfloat16, jnp.float32
    unit = (N_FS, TT, 128)
    args = (tokens, norm_gain.reshape(1, D), gate_weight.T, up_weight.T, down_weight)
    any_spec = pl.BlockSpec(memory_space=pltpu.HBM)
    return pl.pallas_call(
        kernel,
        out_shape=jax.ShapeDtypeStruct((TT, D), bf),
        in_specs=[any_spec] * 5,
        out_specs=pl.BlockSpec(memory_space=pltpu.VMEM),
        scratch_shapes=[
            vmem((4, TT, D), bf), vmem((N_FS, 4 * TT, 128), bf), vmem((N_FS, 2, 2 * F, 128), bf), vmem((N_FS, 2, F, 128), bf),
            vmem((11, 4 * TT, 256), f32), vmem((4 * TT, 2 * F), bf),
            vmem(unit, bf), vmem(unit, bf), vmem(unit, bf), vmem(unit, bf), vmem((2, *unit), bf), vmem(unit, f32),
            dma((4,)), dma((4,)), dma((16,)), dma((16,)), dma((4,)), dma((9,)), dma((18,)), dma((7,)), vmem((1, D), f32),
        ],
        compiler_params=pltpu.CompilerParams(collective_id=0, has_side_effects=True, vmem_limit_bytes=52 * 2**20),
        name="ffn",
    )(*(pltpu.with_memory_space_constraint(a, pltpu.HBM) for a in args))


def solution(mesh):
    placed = (P("fs", None), P(), P("fs", "tp"), P("fs", "tp"), P("tp", "fs"))
    return jax.shard_map(
        per_device, mesh=mesh, in_specs=placed, out_specs=P(("fs", "tp"), None), check_vma=False
    )
```
